32 devices in a mesh: grp: 2 (over y), sp: 4 (over z), tp: 4 (over x, core).
Axes of the slice: x: 2, y: 2, z: 4, core: 2. Of those that a mesh axis runs over, the one named last changes fastest.
Arguments:
- hidden_in: bfloat16 [2048, 2048], P(('grp', 'sp')), parts along dimension 0, may hold values from -6 to 6
- query_latent_rows: bfloat16 [2048, 768], P(('grp', 'sp')), parts along dimension 0, may hold values from -6 to 6
- key_value_latent: bfloat16 [2048, 512], P(('grp', 'sp')), parts along dimension 0, may hold values from -6 to 6
- rotary_key: bfloat16 [2048, 32], P(('grp', 'sp')), parts along dimension 0, may hold values from -64 to 64
- query_norm_gain: float32 [768], replicated, may hold values from 0.1 to 1.9
- key_value_gain: float32 [512], replicated, may hold values from 0.1 to 1.9
- query_up_weight: bfloat16 [768, 1536], P(None, 'tp'), may hold values from -0.625 to 0.625
- key_value_up_weight: bfloat16 [512, 2048], P(None, 'tp'), may hold values from -0.25 to 0.25
- out_proj: bfloat16 [1024, 2048], P('tp'), may hold values from -0.1875 to 0.1875
- feed_gain: float32 [2048], replicated, may hold values from 0.1 to 1.9
- feed_up: bfloat16 [2048, 8192], P('sp', 'tp'), may hold values from -0.125 to 0.125
- feed_down: bfloat16 [8192, 2048], P('tp', 'sp'), may hold values from -0.0625 to 0.0625
Outputs:
- layer_out: bfloat16 [2048, 2048], P(('grp', 'sp', 'tp')), parts along dimension 0
The draws below stay inside these ranges and needn't reach their ends.
There are 2 independent parts, one for each index of `grp`. The reference program is written for one: setup_inputs(seed, part) draws one part's arguments, and reference() takes and returns one part's arrays. A program takes and returns all parts, laid end to end along the dimension named above; an argument that names none is the same for every part. Nothing has to cross between parts.
All inputs are finite; a program needn't handle non-finite values.
Results may differ from the reference program's by a relative error of at most 0.02.
Values may be sent and summed in bfloat16 or wider, within the bound.
A program may use at most 128 MiB of HBM per device.

```python
import math
import jax
import jax.numpy as jnp
from jax import lax

D = 2048
HEAD_COUNT = 16
QUERY_KEY_PLAIN = 64
QUERY_KEY_ROTARY = 32
VALUE_HEAD_SIZE = 64
QUERY_RANK = 768
KEY_VALUE_RANK = 512
FF = 8192
TOKEN_COUNT = 1024


def draw_rotary_key(key, part):
    base = jax.random.normal(jax.random.fold_in(key, 11), (TOKEN_COUNT, QUERY_KEY_ROTARY), jnp.float32)
    return jnp.clip(base, -64.0, 64.0).astype(jnp.bfloat16)


def levels(stream_key, shape, shards, smallest, largest):
    level = 1.0
    for axis_at, blocks in shards:
        heights = jax.random.uniform(jax.random.fold_in(jax.random.fold_in(stream_key, 6), axis_at), (blocks,), jnp.float32, smallest / len(shards), largest / len(shards))
        level = level * jnp.repeat(jnp.exp(heights), shape[axis_at] // blocks).reshape((-1,) + (1,) * (len(shape) - 1 - axis_at))
    return level


def centred(stream_key, extent, deviation, limit, shards=(), kind=jnp.bfloat16):
    factor_of = levels(stream_key, extent, shards, -0.22, 0.18) if shards else 1.0
    drawn = jax.random.normal(stream_key, extent, jnp.float32) * deviation * factor_of
    return jnp.minimum(jnp.maximum(drawn, -limit), limit).astype(kind)


def setup_inputs(seed: int = 0, part: int = 0) -> dict:
    streams_of = jax.random.split(jax.random.key(seed), 13)
    part_keys = jax.random.split(jax.random.fold_in(streams_of[12], part), 13)
    hidden_in = centred(part_keys[0], (TOKEN_COUNT, D), 1.0, 6.0, ((0, 4),))
    query_latent_rows = centred(part_keys[1], (TOKEN_COUNT, QUERY_RANK), 1.0, 6.0, ((0, 4),))
    key_value_latent = centred(part_keys[2], (TOKEN_COUNT, KEY_VALUE_RANK), 1.0, 6.0, ((0, 4),))
    rotary_key = draw_rotary_key(jax.random.fold_in(jax.random.fold_in(streams_of[12], part), 71), part)
    query_norm_gain = jnp.clip(1.0 + 0.18 * jax.random.normal(streams_of[4], (QUERY_RANK,), jnp.float32), 0.1, 1.9)
    key_value_gain = jnp.clip(1.0 + 0.18 * jax.random.normal(streams_of[5], (KEY_VALUE_RANK,), jnp.float32), 0.1, 1.9)
    query_up_weight = centred(streams_of[6], (QUERY_RANK, HEAD_COUNT * (QUERY_KEY_PLAIN + QUERY_KEY_ROTARY)), (3 * QUERY_RANK ** -0.5), 0.625, ((1, 4),))
    key_value_up_weight = centred(streams_of[7], (KEY_VALUE_RANK, HEAD_COUNT * (QUERY_KEY_PLAIN + VALUE_HEAD_SIZE)), KEY_VALUE_RANK ** -0.5, 0.25, ((1, 4),))
    out_proj = centred(streams_of[8], (HEAD_COUNT * VALUE_HEAD_SIZE, D), (HEAD_COUNT * VALUE_HEAD_SIZE) ** -0.5, 0.1875, ((0, 4),))
    feed_gain = jnp.clip(1.0 + 0.18 * jax.random.normal(streams_of[9], (D,), jnp.float32), 0.1, 1.9)
    feed_up = centred(streams_of[10], (D, FF), D ** -0.5, 0.125, ((0, 4), (1, 4)))
    feed_down = centred(streams_of[11], (FF, D), FF ** -0.5, 0.0625, ((0, 4), (1, 4)))
    return {"hidden_in": hidden_in, "query_latent_rows": query_latent_rows, "key_value_latent": key_value_latent, "rotary_key": rotary_key, "query_norm_gain": query_norm_gain, "key_value_gain": key_value_gain, "query_up_weight": query_up_weight, "key_value_up_weight": key_value_up_weight, "out_proj": out_proj, "feed_gain": feed_gain, "feed_up": feed_up, "feed_down": feed_down}


def normalize(values, gain):
    floats = values.astype(jnp.float32)
    return floats * lax.rsqrt(lax.optimization_barrier(jnp.mean(floats * floats, axis=-1, keepdims=True)) + 1e-06) * gain.astype(jnp.float32)

def rotate(values, position):
    half_size = values.shape[-1] // 2
    inverse = 10000.0 ** (-jnp.arange(half_size, dtype=jnp.float32) * 2.0 / values.shape[-1])
    angles = position[:, None] * inverse[None, :]
    cosine = jnp.concatenate([jnp.cos(angles), jnp.cos(angles)], axis=-1)
    sine = jnp.concatenate([jnp.sin(angles), jnp.sin(angles)], axis=-1)
    shape = (values.shape[0],) + (1,) * (values.ndim - 2) + (values.shape[-1],)
    turned = jnp.concatenate([-values[..., half_size:], values[..., :half_size]], axis=-1)
    return values * cosine.reshape(shape) + turned * sine.reshape(shape)

def reference(hidden_in, query_latent_rows, key_value_latent, rotary_key, query_norm_gain, key_value_gain, query_up_weight, key_value_up_weight, out_proj, feed_gain, feed_up, feed_down):
    position = jnp.arange(TOKEN_COUNT).astype(jnp.float32)
    scale_factor = (QUERY_KEY_PLAIN + QUERY_KEY_ROTARY) ** (-0.5)
    query_norm = normalize(query_latent_rows, query_norm_gain).astype(jnp.bfloat16)
    queries = jnp.dot(query_norm, query_up_weight, preferred_element_type=jnp.float32).reshape(TOKEN_COUNT, HEAD_COUNT, QUERY_KEY_PLAIN + QUERY_KEY_ROTARY)
    queries = jnp.concatenate([queries[..., :QUERY_KEY_PLAIN], rotate(queries[..., QUERY_KEY_PLAIN:], position)], axis=-1).astype(jnp.bfloat16)
    latent = normalize(key_value_latent, key_value_gain).astype(jnp.bfloat16)
    keys_values = jnp.dot(latent, key_value_up_weight, preferred_element_type=jnp.float32).astype(jnp.bfloat16)
    keys_values = keys_values.reshape(TOKEN_COUNT, HEAD_COUNT, QUERY_KEY_PLAIN + VALUE_HEAD_SIZE)
    key_nope = keys_values[..., :QUERY_KEY_PLAIN].astype(jnp.float32)
    value_rows = keys_values[..., QUERY_KEY_PLAIN:].astype(jnp.float32)
    key_rope = rotate(rotary_key.astype(jnp.float32), position).astype(jnp.bfloat16).astype(jnp.float32)
    block = math.gcd(TOKEN_COUNT, 512)
    query_blocks = queries.reshape(TOKEN_COUNT // block, block, HEAD_COUNT, QUERY_KEY_PLAIN + QUERY_KEY_ROTARY)

    def attend(query_block):
        plain = query_block[..., :QUERY_KEY_PLAIN].astype(jnp.float32)
        turned = query_block[..., QUERY_KEY_PLAIN:].astype(jnp.float32)
        scores = jnp.einsum('qhd,khd->hqk', plain, key_nope) + jnp.einsum('qhd,kd->hqk', turned, key_rope)
        scores = scores * scale_factor
        expo = jnp.exp(scores - lax.optimization_barrier(jnp.max(scores, axis=-1, keepdims=True)))
        total = lax.optimization_barrier(jnp.sum(expo, axis=-1))
        weights = expo.astype(jnp.bfloat16).astype(jnp.float32)
        summed = jnp.einsum('hqk,khd->qhd', weights, value_rows)
        return summed / jnp.transpose(total)[:, :, None]
    mixed = lax.map(attend, query_blocks).reshape(TOKEN_COUNT, HEAD_COUNT * VALUE_HEAD_SIZE).astype(jnp.bfloat16)
    branch = jnp.dot(mixed, out_proj, preferred_element_type=jnp.float32)
    middle = (hidden_in.astype(jnp.float32) + branch).astype(jnp.bfloat16)
    normed = normalize(middle, feed_gain).astype(jnp.bfloat16)
    upward = jnp.dot(normed, feed_up, preferred_element_type=jnp.float32)
    activated = jnp.square(jax.nn.relu(upward)).astype(jnp.bfloat16)
    feed = jnp.dot(activated, feed_down, preferred_element_type=jnp.float32)
    return (middle.astype(jnp.float32) + feed).astype(jnp.bfloat16)
```

```python
import math

import jax
import jax.numpy as jnp
from jax import lax
from jax.sharding import PartitionSpec as P

QUERY_KEY_PLAIN = 64
QUERY_KEY_ROTARY = 32
VALUE_HEAD_SIZE = 64


def normalize(values, gain):
    floats = values.astype(jnp.float32)
    return floats * lax.rsqrt(jnp.mean(floats * floats, axis=-1, keepdims=True) + 1e-06) * gain


def rotate(values, position):
    half_size = values.shape[-1] // 2
    inverse = 10000.0 ** (-jnp.arange(half_size, dtype=jnp.float32) * 2.0 / values.shape[-1])
    angles = position[:, None] * inverse[None, :]
    cosine = jnp.concatenate([jnp.cos(angles), jnp.cos(angles)], axis=-1)
    sine = jnp.concatenate([jnp.sin(angles), jnp.sin(angles)], axis=-1)
    shape = (values.shape[0],) + (1,) * (values.ndim - 2) + (values.shape[-1],)
    turned = jnp.concatenate([-values[..., half_size:], values[..., :half_size]], axis=-1)
    return values * cosine.reshape(shape) + turned * sine.reshape(shape)


def on_device(
    hidden_in,
    query_latent_rows,
    key_value_latent,
    rotary_key,
    query_norm_gain,
    key_value_gain,
    query_up_weight,
    key_value_up_weight,
    out_proj,
    feed_gain,
    feed_up,
    feed_down,
):
    tokens_here = hidden_in.shape[0]
    heads_here = query_up_weight.shape[1] // (QUERY_KEY_PLAIN + QUERY_KEY_ROTARY)
    position = (lax.axis_index("sp") * tokens_here + jnp.arange(tokens_here)).astype(jnp.float32)
    scale_factor = (QUERY_KEY_PLAIN + QUERY_KEY_ROTARY) ** (-0.5)
    query_norm = normalize(query_latent_rows, query_norm_gain).astype(jnp.bfloat16)
    queries = jnp.dot(query_norm, query_up_weight, preferred_element_type=jnp.float32).reshape(
        tokens_here, heads_here, QUERY_KEY_PLAIN + QUERY_KEY_ROTARY
    )
    queries = jnp.concatenate(
        [queries[..., :QUERY_KEY_PLAIN], rotate(queries[..., QUERY_KEY_PLAIN:], position)], axis=-1
    ).astype(jnp.bfloat16)
    query_plain = queries[..., :QUERY_KEY_PLAIN]
    query_turned = queries[..., QUERY_KEY_PLAIN:]
    latent = normalize(key_value_latent, key_value_gain).astype(jnp.bfloat16)
    key_rope = rotate(rotary_key.astype(jnp.float32), position).astype(jnp.bfloat16)

    def attend_block(carry, key_plain, value_rows, rope_rows):
        row_max, denom, accum = carry
        scores = jnp.einsum(
            "qhd,khd->hqk", query_plain, key_plain, preferred_element_type=jnp.float32
        )
        scores = scores + jnp.einsum(
            "qhd,kd->hqk", query_turned, rope_rows, preferred_element_type=jnp.float32
        )
        scores = scores * scale_factor
        new_max = jnp.maximum(row_max, jnp.max(scores, axis=-1))
        expo = jnp.exp(scores - new_max[:, :, None])
        factor = jnp.exp(row_max - new_max)
        denom = denom * factor + jnp.sum(expo, axis=-1)
        update = jnp.einsum(
            "hqk,khd->qhd",
            expo.astype(jnp.bfloat16),
            value_rows,
            preferred_element_type=jnp.float32,
        )
        accum = accum * jnp.transpose(factor)[:, :, None] + update
        return (new_max, denom, accum)

    start_carry = (
        jnp.full((heads_here, tokens_here), -1e30, jnp.float32),
        jnp.zeros((heads_here, tokens_here), jnp.float32),
        jnp.zeros((tokens_here, heads_here, VALUE_HEAD_SIZE), jnp.float32),
    )
    own_keys = jnp.dot(latent, key_value_up_weight, preferred_element_type=jnp.float32).astype(
        jnp.bfloat16
    )
    pieces = (
        lax.all_gather(own_keys, "sp", axis=0, tiled=True),
        lax.all_gather(key_rope, "sp", axis=0, tiled=True),
    )
    rows_in = pieces[0].shape[0]
    block = math.gcd(rows_in, 1024)

    def step_block(index, inner):
        first = index * block
        bulk = lax.dynamic_slice_in_dim(pieces[0], first, block, 0)
        rope_rows = lax.dynamic_slice_in_dim(pieces[1], first, block, 0)
        bulk = bulk.reshape(block, heads_here, QUERY_KEY_PLAIN + VALUE_HEAD_SIZE)
        return attend_block(
            inner, bulk[..., :QUERY_KEY_PLAIN], bulk[..., QUERY_KEY_PLAIN:], rope_rows
        )

    final_carry = lax.fori_loop(0, rows_in // block, step_block, start_carry)
    denom = final_carry[1]
    accum = final_carry[2]
    mixed = (
        (accum / jnp.transpose(denom)[:, :, None])
        .astype(jnp.bfloat16)
        .reshape(tokens_here, heads_here * VALUE_HEAD_SIZE)
    )
    up_own = lax.all_to_all(feed_up, "sp", split_axis=1, concat_axis=0, tiled=True)
    down_own = lax.all_to_all(feed_down, "sp", split_axis=0, concat_axis=1, tiled=True)
    share = tokens_here // lax.axis_size("tp")
    lead = lax.axis_index("tp") * share
    branch = lax.psum_scatter(
        jnp.dot(mixed, out_proj, preferred_element_type=jnp.float32).astype(jnp.bfloat16),
        "tp",
        scatter_dimension=0,
        tiled=True,
    ).astype(jnp.float32)
    hidden_own = lax.dynamic_slice_in_dim(hidden_in, lead, share, 0)
    middle_own = (hidden_own.astype(jnp.float32) + branch).astype(jnp.bfloat16)
    normed_own = normalize(middle_own, feed_gain).astype(jnp.bfloat16)
    normed = lax.all_gather(normed_own, ("sp", "tp"), axis=0, tiled=True)
    upward = jnp.dot(normed, up_own, preferred_element_type=jnp.float32)
    activated = jnp.square(jax.nn.relu(upward)).astype(jnp.bfloat16)
    partial_sum = jnp.dot(activated, down_own, preferred_element_type=jnp.float32)
    feed = lax.psum_scatter(
        partial_sum.astype(jnp.bfloat16), ("sp", "tp"), scatter_dimension=0, tiled=True
    ).astype(jnp.float32)
    return (middle_own.astype(jnp.float32) + feed).astype(jnp.bfloat16)


def solution(mesh):
    return jax.shard_map(
        on_device,
        mesh=mesh,
        in_specs=(
            P(("grp", "sp"), None),
            P(("grp", "sp"), None),
            P(("grp", "sp"), None),
            P(("grp", "sp"), None),
            P(),
            P(),
            P(None, "tp"),
            P(None, "tp"),
            P("tp", None),
            P(),
            P("sp", "tp"),
            P("tp", "sp"),
        ),
        out_specs=P(("grp", "sp", "tp"), None),
        check_vma=False,
    )
```

```python
import math

import jax
import jax.numpy as jnp
from jax import lax
from jax.experimental import pallas as pl
from jax.experimental.pallas import tpu as pltpu
from jax.sharding import PartitionSpec as P

QUERY_KEY_PLAIN = 64
QUERY_KEY_ROTARY = 32
VALUE_HEAD_SIZE = 64


def normalize(values, gain):
    floats = values.astype(jnp.float32)
    return floats * lax.rsqrt(jnp.mean(floats * floats, axis=-1, keepdims=True) + 1e-06) * gain


def rotate(values, position):
    half_size = values.shape[-1] // 2
    inverse = 10000.0 ** (-jnp.arange(half_size, dtype=jnp.float32) * 2.0 / values.shape[-1])
    angles = position[:, None] * inverse[None, :]
    cosine = jnp.concatenate([jnp.cos(angles), jnp.cos(angles)], axis=-1)
    sine = jnp.concatenate([jnp.sin(angles), jnp.sin(angles)], axis=-1)
    shape = (values.shape[0],) + (1,) * (values.ndim - 2) + (values.shape[-1],)
    turned = jnp.concatenate([-values[..., half_size:], values[..., :half_size]], axis=-1)
    return values * cosine.reshape(shape) + turned * sine.reshape(shape)


MESH = pl.DeviceIdType.MESH


def layer_kernel(
    n, heads, qp, qr, kvr, hidden, op, gain, up, down, out,
    kv_all, op_pad, mixed, up_all, down_all, part_d, recv_d, middle, norm_all, act, part,
    rf1, c2, rf2, c3, rf3, ss, rs, ls,
):
    g, me, t = lax.axis_index("grp"), lax.axis_index("sp"), lax.axis_index("tp")
    c, x = lax.rem(t, 2), t // 2
    rows = kvr.shape[0]
    share, width = middle.shape
    piece_k = up.shape[0]
    hid = down_all.shape[0]
    half_k, half_h = piece_k // 2, hid // 2
    wide = down.shape[1]
    scale_factor = (QUERY_KEY_PLAIN + QUERY_KEY_ROTARY) ** (-0.5)

    def at_z(k):
        return lax.rem(me + k, n)

    def from_z(k):
        return lax.rem(me - k + n, n)

    def at_tp(cc, xx):
        return {"tp": xx * 2 + cc}

    sib, xpeer, ypeer = at_tp(1 - c, x), at_tp(c, 1 - x), {"grp": 1 - g}
    barrier = pltpu.get_barrier_semaphore()
    for k in range(1, n):
        pl.semaphore_signal(barrier, inc=1, device_id={"sp": at_z(k)}, device_id_type=MESH)
    for peer in (sib, xpeer, at_tp(1 - c, 1 - x), ypeer):
        pl.semaphore_signal(barrier, inc=1, device_id=peer, device_id_type=MESH)
    pl.semaphore_wait(barrier, n + 3)

    names = {}
    sent = []

    def slot(name):
        if name not in names:
            names[name] = len(names)
        return names[name]

    def send(name, src, dst, dev):
        i = slot(name)
        copy = pltpu.make_async_remote_copy(
            src_ref=src, dst_ref=dst, send_sem=ss.at[i], recv_sem=rs.at[i],
            device_id=dev, device_id_type=MESH,
        )
        copy.start()
        sent.append(copy)

    def land(name, dst):
        i = slot(name)
        pltpu.make_async_remote_copy(
            src_ref=dst, dst_ref=dst, send_sem=ss.at[i], recv_sem=rs.at[i],
            device_id=sib, device_id_type=MESH,
        ).wait_recv()

    def up_half(owner, hv):
        return up_all.at[pl.ds(pl.multiple_of(owner * piece_k + hv * half_k, half_k), half_k)]

    def down_half(owner, hv):
        return down_all.at[
            pl.ds(pl.multiple_of(hv * half_h, half_h), half_h),
            pl.ds(pl.multiple_of(owner * wide, wide), wide),
        ]

    for k in range(1, n):
        send(("kv", k), kvr, kv_all.at[me], {"sp": at_z(k)})
    for k in range(1, n):
        send(
            ("up", k),
            up.at[
                pl.ds(pl.multiple_of(g * half_k, half_k), half_k),
                pl.ds(pl.multiple_of(at_z(k) * hid, hid), hid),
            ],
            up_half(me, g),
            {"sp": at_z(k)},
        )
    local = [
        pltpu.make_async_copy(
            up.at[:, pl.ds(pl.multiple_of(me * hid, hid), hid)],
            up_all.at[pl.ds(pl.multiple_of(me * piece_k, piece_k), piece_k)],
            ls.at[0],
        ),
        pltpu.make_async_copy(
            down.at[pl.ds(pl.multiple_of(me * hid, hid), hid)],
            down_all.at[:, pl.ds(pl.multiple_of(me * wide, wide), wide)],
            ls.at[1],
        ),
    ]
    for copy in local:
        copy.start()
    kv_all[me] = kvr[...]
    vh = VALUE_HEAD_SIZE
    unit = QUERY_KEY_PLAIN + vh
    for h in range(heads):
        op_pad[h * unit : h * unit + QUERY_KEY_PLAIN] = jnp.zeros((QUERY_KEY_PLAIN, width), op.dtype)
        op_pad[h * unit + QUERY_KEY_PLAIN : (h + 1) * unit] = op[h * vh : (h + 1) * vh]
    for k in range(1, n):
        land(("kv", k), kv_all.at[from_z(k)])

    contract = (((1,), (1,)), ((), ()))
    rope = kv_all[:, :, heads * unit :].reshape(n * rows, -1)
    for h in range(heads):
        kv = kv_all[:, :, h * unit : (h + 1) * unit].reshape(n * rows, unit)
        scores = lax.dot_general(qp[h], kv, contract, preferred_element_type=jnp.float32)
        scores += lax.dot_general(qr[h], rope, contract, preferred_element_type=jnp.float32)
        scores = scores * scale_factor
        expo = jnp.exp(scores - jnp.max(scores, axis=-1, keepdims=True))
        total = jnp.sum(expo, axis=-1, keepdims=True)
        mix = jnp.dot(expo.astype(jnp.bfloat16), kv, preferred_element_type=jnp.float32)
        mixed[:, h * unit : (h + 1) * unit] = (mix / total).astype(jnp.bfloat16)

    tile = math.gcd(width, 512)

    @pl.loop(0, width // tile)
    def _(j):
        cols = pl.ds(pl.multiple_of(j * tile, tile), tile)
        part_d[:, cols] = jnp.dot(
            mixed[...], op_pad[:, cols], preferred_element_type=jnp.float32
        ).astype(jnp.bfloat16)

    def own_rows(cc, xx):
        return pl.ds(pl.multiple_of((xx * 2 + cc) * share, share), share)

    others = ((c, 1 - x), (1 - c, 1 - x), (1 - c, x))
    for j, (cc, xx) in enumerate(others):
        send(("d", j), part_d.at[own_rows(cc, xx)], recv_d.at[j], at_tp(cc, xx))
    branch = part_d[own_rows(c, x)].astype(jnp.float32)
    for j in range(3):
        land(("d", j), recv_d.at[j])
        branch += recv_d[j].astype(jnp.float32)
    middle[...] = (hidden[own_rows(c, x)].astype(jnp.float32) + branch).astype(jnp.bfloat16)
    norm_all[me, c, x] = normalize(middle[...], gain[...]).astype(jnp.bfloat16)

    own = norm_all.at[me, c, x]
    for k in range(1, n):
        send(("nz", k), own, own, {"sp": at_z(k)})
    send(("nx", 0), own, own, xpeer)
    send(("ns", 0), own, own, sib)
    for k in range(1, n):
        send(
            ("dn", k),
            down.at[pl.ds(pl.multiple_of(at_z(k) * hid + g * half_h, half_h), half_h)],
            down_half(me, g),
            {"sp": at_z(k)},
        )
    for k in range(1, n):
        piece = up_half(from_z(k), g)
        land(("up", k), piece)
        send(("uy", k), piece, piece, ypeer)
    for k in range(1, n):
        piece = norm_all.at[from_z(k), c, x]
        land(("nz", k), piece)
        send(("nx", k), piece, piece, xpeer)
        send(("ns", k), piece, piece, sib)
    for k in range(n):
        piece = norm_all.at[from_z(k), c, 1 - x]
        land(("nx", k), piece)
        send(("nt", k), piece, piece, sib)
    for k in range(1, n):
        land(("uy", k), up_half(from_z(k), 1 - g))
    local[0].wait()
    for k in range(n):
        land(("ns", k), norm_all.at[from_z(k), 1 - c, x])
        land(("nt", k), norm_all.at[from_z(k), 1 - c, 1 - x])

    @pl.loop(0, n)
    def _(j):
        upward = jnp.dot(
            norm_all[j].reshape(rows, width), up_all[...], preferred_element_type=jnp.float32
        )
        act[j] = jnp.square(jnp.maximum(upward, 0.0)).astype(jnp.bfloat16)

    for k in range(1, n):
        piece = down_half(from_z(k), g)
        land(("dn", k), piece)
        send(("dy", k), piece, piece, ypeer)
    for k in range(1, n):
        land(("dy", k), down_half(from_z(k), 1 - g))
    local[1].wait()

    order = [*range(1, n), 0]
    for k in order:
        dest = at_z(k)

        @pl.loop(0, width // tile)
        def _(j):
            cols = pl.ds(pl.multiple_of(j * tile, tile), tile)
            made = jnp.dot(act[dest], down_all[:, cols], preferred_element_type=jnp.float32)
            part[k, :, :, :, cols] = made.astype(jnp.bfloat16).reshape(2, 2, share, tile)

        send(("f1", k), part.at[k, 1 - c], rf1.at[k], sib)
    for k in order:
        land(("f1", k), rf1.at[k])
        c2[k] = (
            part[k, c, 1 - x].astype(jnp.float32) + rf1[k, 1 - x].astype(jnp.float32)
        ).astype(jnp.bfloat16)
        send(("f2", k), c2.at[k], rf2.at[k], xpeer)
    for k in order:
        land(("f2", k), rf2.at[k])
        c3[k] = (
            part[k, c, x].astype(jnp.float32)
            + rf1[k, x].astype(jnp.float32)
            + rf2[k].astype(jnp.float32)
        ).astype(jnp.bfloat16)
        if k:
            send(("f3", k), c3.at[k], rf3.at[k], {"sp": at_z(k)})
    feed = c3[0].astype(jnp.float32)
    for k in range(1, n):
        land(("f3", k), rf3.at[k])
        feed += rf3[k].astype(jnp.float32)
    out[...] = (middle[...].astype(jnp.float32) + feed).astype(jnp.bfloat16)
    for copy in sent:
        copy.wait_send()


def run_layer(queries, own_keys, key_rope, hidden_in, out_proj, feed_gain, feed_up, feed_down):
    n = lax.axis_size("sp")
    rows, heads, size = queries.shape
    width = hidden_in.shape[1]
    share = rows // lax.axis_size("tp")
    hid = feed_up.shape[1] // n
    turned = jnp.transpose(queries, (1, 0, 2))
    unit = QUERY_KEY_PLAIN + VALUE_HEAD_SIZE
    plain = jnp.pad(turned[..., :QUERY_KEY_PLAIN], ((0, 0), (0, 0), (0, VALUE_HEAD_SIZE)))
    rotary = jnp.pad(turned[..., QUERY_KEY_PLAIN:], ((0, 0), (0, 0), (0, unit - QUERY_KEY_ROTARY)))
    kvr = jnp.concatenate(
        [own_keys, jnp.pad(key_rope, ((0, 0), (0, unit - QUERY_KEY_ROTARY)))], axis=1
    )
    bf = jnp.bfloat16
    vmem = pl.BlockSpec(memory_space=pltpu.VMEM)
    anywhere = pl.BlockSpec(memory_space=pl.ANY)
    copies = 12 * n
    block = (share, width)
    return pl.pallas_call(
        lambda *refs: layer_kernel(n, heads, *refs),
        out_shape=jax.ShapeDtypeStruct(block, bf),
        in_specs=[vmem] * 6 + [anywhere] * 2,
        out_specs=vmem,
        scratch_shapes=[
            pltpu.VMEM((n, *kvr.shape), bf),
            pltpu.VMEM((heads * unit, width), bf),
            pltpu.VMEM((rows, heads * unit), bf),
            pltpu.VMEM((feed_up.shape[0] * n, hid), bf),
            pltpu.VMEM((hid, feed_down.shape[1] * n), bf),
            pltpu.VMEM((rows, width), bf),
            pltpu.VMEM((3, *block), bf),
            pltpu.VMEM(block, bf),
            pltpu.VMEM((n, 2, 2, *block), bf),
            pltpu.VMEM((n, rows, hid), bf),
            pltpu.VMEM((n, 2, 2, *block), bf),
            pltpu.VMEM((n, 2, *block), bf),
            pltpu.VMEM((n, *block), bf),
            pltpu.VMEM((n, *block), bf),
            pltpu.VMEM((n, *block), bf),
            pltpu.VMEM((n, *block), bf),
            pltpu.SemaphoreType.DMA((copies,)),
            pltpu.SemaphoreType.DMA((copies,)),
            pltpu.SemaphoreType.DMA((2,)),
        ],
        compiler_params=pltpu.CompilerParams(
            collective_id=0, has_side_effects=True, vmem_limit_bytes=60 * 1024 * 1024
        ),
    )(plain, rotary, kvr, hidden_in, out_proj, feed_gain.reshape(1, -1), feed_up, feed_down)


def fits_kernel(tokens, feed_up):
    n = lax.axis_size("sp")
    hid = feed_up.shape[1] // n
    return (
        lax.axis_size("grp") == 2
        and lax.axis_size("tp") == 4
        and 1 < n
        and tokens * n <= 1024
        and tokens % 64 == 0
        and hid % 128 == 0
        and hid <= 512
    )


def on_device(
    hidden_in,
    query_latent_rows,
    key_value_latent,
    rotary_key,
    query_norm_gain,
    key_value_gain,
    query_up_weight,
    key_value_up_weight,
    out_proj,
    feed_gain,
    feed_up,
    feed_down,
):
    tokens_here = hidden_in.shape[0]
    heads_here = query_up_weight.shape[1] // (QUERY_KEY_PLAIN + QUERY_KEY_ROTARY)
    position = (lax.axis_index("sp") * tokens_here + jnp.arange(tokens_here)).astype(jnp.float32)
    scale_factor = (QUERY_KEY_PLAIN + QUERY_KEY_ROTARY) ** (-0.5)
    query_norm = normalize(query_latent_rows, query_norm_gain).astype(jnp.bfloat16)
    queries = jnp.dot(query_norm, query_up_weight, preferred_element_type=jnp.float32).reshape(
        tokens_here, heads_here, QUERY_KEY_PLAIN + QUERY_KEY_ROTARY
    )
    queries = jnp.concatenate(
        [queries[..., :QUERY_KEY_PLAIN], rotate(queries[..., QUERY_KEY_PLAIN:], position)], axis=-1
    ).astype(jnp.bfloat16)
    query_plain = queries[..., :QUERY_KEY_PLAIN]
    query_turned = queries[..., QUERY_KEY_PLAIN:]
    latent = normalize(key_value_latent, key_value_gain).astype(jnp.bfloat16)
    key_rope = rotate(rotary_key.astype(jnp.float32), position).astype(jnp.bfloat16)

    def attend_block(carry, key_plain, value_rows, rope_rows):
        row_max, denom, accum = carry
        scores = jnp.einsum(
            "qhd,khd->hqk", query_plain, key_plain, preferred_element_type=jnp.float32
        )
        scores = scores + jnp.einsum(
            "qhd,kd->hqk", query_turned, rope_rows, preferred_element_type=jnp.float32
        )
        scores = scores * scale_factor
        new_max = jnp.maximum(row_max, jnp.max(scores, axis=-1))
        expo = jnp.exp(scores - new_max[:, :, None])
        factor = jnp.exp(row_max - new_max)
        denom = denom * factor + jnp.sum(expo, axis=-1)
        update = jnp.einsum(
            "hqk,khd->qhd",
            expo.astype(jnp.bfloat16),
            value_rows,
            preferred_element_type=jnp.float32,
        )
        accum = accum * jnp.transpose(factor)[:, :, None] + update
        return (new_max, denom, accum)

    start_carry = (
        jnp.full((heads_here, tokens_here), -1e30, jnp.float32),
        jnp.zeros((heads_here, tokens_here), jnp.float32),
        jnp.zeros((tokens_here, heads_here, VALUE_HEAD_SIZE), jnp.float32),
    )
    own_keys = jnp.dot(latent, key_value_up_weight, preferred_element_type=jnp.float32).astype(
        jnp.bfloat16
    )
    if fits_kernel(tokens_here, feed_up):
        return run_layer(
            queries, own_keys, key_rope, hidden_in, out_proj, feed_gain, feed_up, feed_down
        )
    pieces = (
        lax.all_gather(own_keys, "sp", axis=0, tiled=True),
        lax.all_gather(key_rope, "sp", axis=0, tiled=True),
    )
    rows_in = pieces[0].shape[0]
    block = math.gcd(rows_in, 1024)

    def step_block(index, inner):
        first = index * block
        bulk = lax.dynamic_slice_in_dim(pieces[0], first, block, 0)
        rope_rows = lax.dynamic_slice_in_dim(pieces[1], first, block, 0)
        bulk = bulk.reshape(block, heads_here, QUERY_KEY_PLAIN + VALUE_HEAD_SIZE)
        return attend_block(
            inner, bulk[..., :QUERY_KEY_PLAIN], bulk[..., QUERY_KEY_PLAIN:], rope_rows
        )

    final_carry = lax.fori_loop(0, rows_in // block, step_block, start_carry)
    denom = final_carry[1]
    accum = final_carry[2]
    mixed = (
        (accum / jnp.transpose(denom)[:, :, None])
        .astype(jnp.bfloat16)
        .reshape(tokens_here, heads_here * VALUE_HEAD_SIZE)
    )
    up_own = lax.all_to_all(feed_up, "sp", split_axis=1, concat_axis=0, tiled=True)
    down_own = lax.all_to_all(feed_down, "sp", split_axis=0, concat_axis=1, tiled=True)
    share = tokens_here // lax.axis_size("tp")
    lead = lax.axis_index("tp") * share
    branch = lax.psum_scatter(
        jnp.dot(mixed, out_proj, preferred_element_type=jnp.float32).astype(jnp.bfloat16),
        "tp",
        scatter_dimension=0,
        tiled=True,
    ).astype(jnp.float32)
    hidden_own = lax.dynamic_slice_in_dim(hidden_in, lead, share, 0)
    middle_own = (hidden_own.astype(jnp.float32) + branch).astype(jnp.bfloat16)
    normed_own = normalize(middle_own, feed_gain).astype(jnp.bfloat16)
    normed = lax.all_gather(normed_own, ("sp", "tp"), axis=0, tiled=True)
    upward = jnp.dot(normed, up_own, preferred_element_type=jnp.float32)
    activated = jnp.square(jax.nn.relu(upward)).astype(jnp.bfloat16)
    partial_sum = jnp.dot(activated, down_own, preferred_element_type=jnp.float32)
    feed = lax.psum_scatter(
        partial_sum.astype(jnp.bfloat16), ("sp", "tp"), scatter_dimension=0, tiled=True
    ).astype(jnp.float32)
    return (middle_own.astype(jnp.float32) + feed).astype(jnp.bfloat16)


def solution(mesh):
    return jax.shard_map(
        on_device,
        mesh=mesh,
        in_specs=(
            P(("grp", "sp"), None),
            P(("grp", "sp"), None),
            P(("grp", "sp"), None),
            P(("grp", "sp"), None),
            P(),
            P(),
            P(None, "tp"),
            P(None, "tp"),
            P("tp", None),
            P(),
            P("sp", "tp"),
            P("tp", "sp"),
        ),
        out_specs=P(("grp", "sp", "tp"), None),
        check_vma=False,
    )
```

```python
import math

import jax
import jax.numpy as jnp
from jax import lax
from jax.experimental import pallas as pl
from jax.experimental.pallas import tpu as pltpu
from jax.sharding import PartitionSpec as P

QUERY_KEY_PLAIN = 64
QUERY_KEY_ROTARY = 32
VALUE_HEAD_SIZE = 64


def normalize(values, gain):
    floats = values.astype(jnp.float32)
    return floats * lax.rsqrt(jnp.mean(floats * floats, axis=-1, keepdims=True) + 1e-06) * gain


def rotate(values, position):
    half_size = values.shape[-1] // 2
    inverse = 10000.0 ** (-jnp.arange(half_size, dtype=jnp.float32) * 2.0 / values.shape[-1])
    angles = position[:, None] * inverse[None, :]
    cosine = jnp.concatenate([jnp.cos(angles), jnp.cos(angles)], axis=-1)
    sine = jnp.concatenate([jnp.sin(angles), jnp.sin(angles)], axis=-1)
    shape = (values.shape[0],) + (1,) * (values.ndim - 2) + (values.shape[-1],)
    turned = jnp.concatenate([-values[..., half_size:], values[..., :half_size]], axis=-1)
    return values * cosine.reshape(shape) + turned * sine.reshape(shape)


MESH = pl.DeviceIdType.MESH


def layer_kernel(
    n, heads, qp, qr, lat, wkv, hidden, op, gain, up, down, out,
    lat_all, kv_all, op_pad, mixed, up_all, down_all, part_d, recv_d, middle, norm_all, act, part,
    rf1, c2, rf2, c3, rf3, ss, rs, ls,
):
    g, me, t = lax.axis_index("grp"), lax.axis_index("sp"), lax.axis_index("tp")
    c, x = lax.rem(t, 2), t // 2
    share, width = middle.shape
    rows = share * 4
    rank = wkv.shape[0]
    piece_k = up.shape[0]
    hid = down_all.shape[0]
    half_k, half_h = piece_k // 2, hid // 2
    wide = down.shape[1]
    scale_factor = (QUERY_KEY_PLAIN + QUERY_KEY_ROTARY) ** (-0.5)

    def at_z(k):
        return lax.rem(me + k, n)

    def from_z(k):
        return lax.rem(me - k + n, n)

    def at_tp(cc, xx):
        return {"tp": xx * 2 + cc}

    sib, xpeer, ypeer = at_tp(1 - c, x), at_tp(c, 1 - x), {"grp": 1 - g}
    barrier = pltpu.get_barrier_semaphore()
    for k in range(1, n):
        pl.semaphore_signal(barrier, inc=1, device_id={"sp": at_z(k)}, device_id_type=MESH)
    for peer in (sib, xpeer, at_tp(1 - c, 1 - x), ypeer):
        pl.semaphore_signal(barrier, inc=1, device_id=peer, device_id_type=MESH)
    pl.semaphore_wait(barrier, n + 3)

    names = {}
    sent = []

    def slot(name):
        if name not in names:
            names[name] = len(names)
        return names[name]

    def send(name, src, dst, dev):
        i = slot(name)
        copy = pltpu.make_async_remote_copy(
            src_ref=src, dst_ref=dst, send_sem=ss.at[i], recv_sem=rs.at[i],
            device_id=dev, device_id_type=MESH,
        )
        copy.start()
        sent.append(copy)

    def land(name, dst):
        i = slot(name)
        pltpu.make_async_remote_copy(
            src_ref=dst, dst_ref=dst, send_sem=ss.at[i], recv_sem=rs.at[i],
            device_id=sib, device_id_type=MESH,
        ).wait_recv()

    def up_half(owner, hv):
        return up_all.at[pl.ds(pl.multiple_of(owner * piece_k + hv * half_k, half_k), half_k)]

    def down_half(owner, hv):
        return down_all.at[
            pl.ds(pl.multiple_of(hv * half_h, half_h), half_h),
            pl.ds(pl.multiple_of(owner * wide, wide), wide),
        ]

    def begin(tag, buf):
        own = buf.at[me, c, x]
        for k in range(1, n):
            send((tag, "z", k), own, own, {"sp": at_z(k)})
        send((tag, "x", 0), own, own, xpeer)
        send((tag, "s", 0), own, own, sib)

    def finish(tag, buf):
        for k in range(1, n):
            piece = buf.at[from_z(k), c, x]
            land((tag, "z", k), piece)
            send((tag, "x", k), piece, piece, xpeer)
            send((tag, "s", k), piece, piece, sib)
        for k in range(n):
            piece = buf.at[from_z(k), c, 1 - x]
            land((tag, "x", k), piece)
            send((tag, "t", k), piece, piece, sib)
        for k in range(n):
            land((tag, "s", k), buf.at[from_z(k), 1 - c, x])
            land((tag, "t", k), buf.at[from_z(k), 1 - c, 1 - x])

    def send_down(k):
        send(
            ("dn", k),
            down.at[pl.ds(pl.multiple_of(at_z(k) * hid + g * half_h, half_h), half_h)],
            down_half(me, g),
            {"sp": at_z(k)},
        )

    lat_all[me, c, x] = lat[...]
    begin("l", lat_all)
    for k in range(1, n):
        send(
            ("up", k),
            up.at[
                pl.ds(pl.multiple_of(g * half_k, half_k), half_k),
                pl.ds(pl.multiple_of(at_z(k) * hid, hid), hid),
            ],
            up_half(me, g),
            {"sp": at_z(k)},
        )
    send_down(1)
    local = [
        pltpu.make_async_copy(
            up.at[:, pl.ds(pl.multiple_of(me * hid, hid), hid)],
            up_all.at[pl.ds(pl.multiple_of(me * piece_k, piece_k), piece_k)],
            ls.at[0],
        ),
        pltpu.make_async_copy(
            down.at[pl.ds(pl.multiple_of(me * hid, hid), hid)],
            down_all.at[:, pl.ds(pl.multiple_of(me * wide, wide), wide)],
            ls.at[1],
        ),
    ]
    for copy in local:
        copy.start()
    vh = VALUE_HEAD_SIZE
    unit = QUERY_KEY_PLAIN + vh
    for h in range(heads):
        op_pad[h * unit : h * unit + QUERY_KEY_PLAIN] = jnp.zeros((QUERY_KEY_PLAIN, width), op.dtype)
        op_pad[h * unit + QUERY_KEY_PLAIN : (h + 1) * unit] = op[h * vh : (h + 1) * vh]
    finish("l", lat_all)
    for j in range(n):
        kv_all[j] = jnp.dot(
            lat_all[j, :, :, :, :rank].reshape(rows, rank),
            wkv[...],
            preferred_element_type=jnp.float32,
        ).astype(jnp.bfloat16)

    contract = (((1,), (1,)), ((), ()))
    rope = lat_all[:, :, :, :, rank:].reshape(n * rows, -1)
    for h in range(heads):
        kv = kv_all[:, :, h * unit : (h + 1) * unit].reshape(n * rows, unit)
        scores = lax.dot_general(qp[h], kv, contract, preferred_element_type=jnp.float32)
        scores += lax.dot_general(qr[h], rope, contract, preferred_element_type=jnp.float32)
        scores = scores * scale_factor
        expo = jnp.exp(scores - jnp.max(scores, axis=-1, keepdims=True))
        total = jnp.sum(expo, axis=-1, keepdims=True)
        mix = jnp.dot(expo.astype(jnp.bfloat16), kv, preferred_element_type=jnp.float32)
        mixed[:, h * unit : (h + 1) * unit] = (mix / total).astype(jnp.bfloat16)

    tile = math.gcd(width, 512)

    @pl.loop(0, width // tile)
    def _(j):
        cols = pl.ds(pl.multiple_of(j * tile, tile), tile)
        part_d[:, cols] = jnp.dot(
            mixed[...], op_pad[:, cols], preferred_element_type=jnp.float32
        ).astype(jnp.bfloat16)

    def own_rows(cc, xx):
        return pl.ds(pl.multiple_of((xx * 2 + cc) * share, share), share)

    others = ((c, 1 - x), (1 - c, 1 - x), (1 - c, x))
    for j, (cc, xx) in enumerate(others):
        send(("d", j), part_d.at[own_rows(cc, xx)], recv_d.at[j], at_tp(cc, xx))
    branch = part_d[own_rows(c, x)].astype(jnp.float32)
    for j in range(3):
        land(("d", j), recv_d.at[j])
        branch += recv_d[j].astype(jnp.float32)
    middle[...] = (hidden[own_rows(c, x)].astype(jnp.float32) + branch).astype(jnp.bfloat16)
    norm_all[me, c, x] = normalize(middle[...], gain[...]).astype(jnp.bfloat16)

    begin("n", norm_all)
    for k in range(2, n):
        send_down(k)
    for k in range(1, n):
        piece = up_half(from_z(k), g)
        land(("up", k), piece)
        send(("uy", k), piece, piece, ypeer)
    finish("n", norm_all)
    for k in range(1, n):
        land(("uy", k), up_half(from_z(k), 1 - g))
    local[0].wait()
    @pl.loop(0, n)
    def _(j):
        upward = jnp.dot(
            norm_all[j].reshape(rows, width), up_all[...], preferred_element_type=jnp.float32
        )
        act[j] = jnp.square(jnp.maximum(upward, 0.0)).astype(jnp.bfloat16)

    for k in range(1, n):
        piece = down_half(from_z(k), g)
        land(("dn", k), piece)
        send(("dy", k), piece, piece, ypeer)
    for k in range(1, n):
        land(("dy", k), down_half(from_z(k), 1 - g))
    local[1].wait()

    order = [*range(1, n), 0]
    for k in order:
        dest = at_z(k)

        @pl.loop(0, width // tile)
        def _(j):
            cols = pl.ds(pl.multiple_of(j * tile, tile), tile)
            made = jnp.dot(act[dest], down_all[:, cols], preferred_element_type=jnp.float32)
            part[k, :, :, :, cols] = made.astype(jnp.bfloat16).reshape(2, 2, share, tile)

        send(("f1", k), part.at[k, 1 - c], rf1.at[k], sib)
    for k in order:
        land(("f1", k), rf1.at[k])
        c2[k] = (
            part[k, c, 1 - x].astype(jnp.float32) + rf1[k, 1 - x].astype(jnp.float32)
        ).astype(jnp.bfloat16)
        send(("f2", k), c2.at[k], rf2.at[k], xpeer)
    for k in order:
        land(("f2", k), rf2.at[k])
        c3[k] = (
            part[k, c, x].astype(jnp.float32)
            + rf1[k, x].astype(jnp.float32)
            + rf2[k].astype(jnp.float32)
        ).astype(jnp.bfloat16)
        if k:
            send(("f3", k), c3.at[k], rf3.at[k], {"sp": at_z(k)})
    feed = c3[0].astype(jnp.float32)
    for k in range(1, n):
        land(("f3", k), rf3.at[k])
        feed += rf3[k].astype(jnp.float32)
    out[...] = (middle[...].astype(jnp.float32) + feed).astype(jnp.bfloat16)
    for copy in sent:
        copy.wait_send()


def run_layer(
    queries, latent, key_rope, key_value_up_weight, hidden_in, out_proj, feed_gain, feed_up, feed_down
):
    n = lax.axis_size("sp")
    rows, heads, size = queries.shape
    width = hidden_in.shape[1]
    share = rows // lax.axis_size("tp")
    hid = feed_up.shape[1] // n
    turned = jnp.transpose(queries, (1, 0, 2))
    unit = QUERY_KEY_PLAIN + VALUE_HEAD_SIZE
    plain = jnp.pad(turned[..., :QUERY_KEY_PLAIN], ((0, 0), (0, 0), (0, VALUE_HEAD_SIZE)))
    rotary = jnp.pad(turned[..., QUERY_KEY_PLAIN:], ((0, 0), (0, 0), (0, unit - QUERY_KEY_ROTARY)))
    lat = jnp.concatenate(
        [latent, jnp.pad(key_rope, ((0, 0), (0, unit - QUERY_KEY_ROTARY)))], axis=1
    )
    lat = lax.dynamic_slice_in_dim(lat, lax.axis_index("tp") * share, share, 0)
    bf = jnp.bfloat16
    vmem = pl.BlockSpec(memory_space=pltpu.VMEM)
    anywhere = pl.BlockSpec(memory_space=pl.ANY)
    copies = 16 * n
    block = (share, width)
    return pl.pallas_call(
        lambda *refs: layer_kernel(n, heads, *refs),
        out_shape=jax.ShapeDtypeStruct(block, bf),
        in_specs=[vmem] * 7 + [anywhere] * 2,
        out_specs=vmem,
        scratch_shapes=[
            pltpu.VMEM((n, 2, 2, *lat.shape), bf),
            pltpu.VMEM((n, rows, heads * unit), bf),
            pltpu.VMEM((heads * unit, width), bf),
            pltpu.VMEM((rows, heads * unit), bf),
            pltpu.VMEM((feed_up.shape[0] * n, hid), bf),
            pltpu.VMEM((hid, feed_down.shape[1] * n), bf),
            pltpu.VMEM((rows, width), bf),
            pltpu.VMEM((3, *block), bf),
            pltpu.VMEM(block, bf),
            pltpu.VMEM((n, 2, 2, *block), bf),
            pltpu.VMEM((n, rows, hid), bf),
            pltpu.VMEM((n, 2, 2, *block), bf),
            pltpu.VMEM((n, 2, *block), bf),
            pltpu.VMEM((n, *block), bf),
            pltpu.VMEM((n, *block), bf),
            pltpu.VMEM((n, *block), bf),
            pltpu.VMEM((n, *block), bf),
            pltpu.SemaphoreType.DMA((copies,)),
            pltpu.SemaphoreType.DMA((copies,)),
            pltpu.SemaphoreType.DMA((2,)),
        ],
        compiler_params=pltpu.CompilerParams(
            collective_id=0, has_side_effects=True, vmem_limit_bytes=60 * 1024 * 1024
        ),
    )(
        plain, rotary, lat, key_value_up_weight, hidden_in, out_proj,
        feed_gain.reshape(1, -1), feed_up, feed_down,
    )


def fits_kernel(tokens, feed_up):
    n = lax.axis_size("sp")
    hid = feed_up.shape[1] // n
    return (
        lax.axis_size("grp") == 2
        and lax.axis_size("tp") == 4
        and 1 < n
        and tokens * n <= 1024
        and tokens % 64 == 0
        and hid % 128 == 0
        and hid <= 512
    )


def on_device(
    hidden_in,
    query_latent_rows,
    key_value_latent,
    rotary_key,
    query_norm_gain,
    key_value_gain,
    query_up_weight,
    key_value_up_weight,
    out_proj,
    feed_gain,
    feed_up,
    feed_down,
):
    tokens_here = hidden_in.shape[0]
    heads_here = query_up_weight.shape[1] // (QUERY_KEY_PLAIN + QUERY_KEY_ROTARY)
    position = (lax.axis_index("sp") * tokens_here + jnp.arange(tokens_here)).astype(jnp.float32)
    scale_factor = (QUERY_KEY_PLAIN + QUERY_KEY_ROTARY) ** (-0.5)
    query_norm = normalize(query_latent_rows, query_norm_gain).astype(jnp.bfloat16)
    queries = jnp.dot(query_norm, query_up_weight, preferred_element_type=jnp.float32).reshape(
        tokens_here, heads_here, QUERY_KEY_PLAIN + QUERY_KEY_ROTARY
    )
    queries = jnp.concatenate(
        [queries[..., :QUERY_KEY_PLAIN], rotate(queries[..., QUERY_KEY_PLAIN:], position)], axis=-1
    ).astype(jnp.bfloat16)
    query_plain = queries[..., :QUERY_KEY_PLAIN]
    query_turned = queries[..., QUERY_KEY_PLAIN:]
    latent = normalize(key_value_latent, key_value_gain).astype(jnp.bfloat16)
    key_rope = rotate(rotary_key.astype(jnp.float32), position).astype(jnp.bfloat16)

    def attend_block(carry, key_plain, value_rows, rope_rows):
        row_max, denom, accum = carry
        scores = jnp.einsum(
            "qhd,khd->hqk", query_plain, key_plain, preferred_element_type=jnp.float32
        )
        scores = scores + jnp.einsum(
            "qhd,kd->hqk", query_turned, rope_rows, preferred_element_type=jnp.float32
        )
        scores = scores * scale_factor
        new_max = jnp.maximum(row_max, jnp.max(scores, axis=-1))
        expo = jnp.exp(scores - new_max[:, :, None])
        factor = jnp.exp(row_max - new_max)
        denom = denom * factor + jnp.sum(expo, axis=-1)
        update = jnp.einsum(
            "hqk,khd->qhd",
            expo.astype(jnp.bfloat16),
            value_rows,
            preferred_element_type=jnp.float32,
        )
        accum = accum * jnp.transpose(factor)[:, :, None] + update
        return (new_max, denom, accum)

    start_carry = (
        jnp.full((heads_here, tokens_here), -1e30, jnp.float32),
        jnp.zeros((heads_here, tokens_here), jnp.float32),
        jnp.zeros((tokens_here, heads_here, VALUE_HEAD_SIZE), jnp.float32),
    )
    own_keys = jnp.dot(latent, key_value_up_weight, preferred_element_type=jnp.float32).astype(
        jnp.bfloat16
    )
    if fits_kernel(tokens_here, feed_up):
        return run_layer(
            queries, latent, key_rope, key_value_up_weight, hidden_in, out_proj,
            feed_gain, feed_up, feed_down,
        )
    pieces = (
        lax.all_gather(own_keys, "sp", axis=0, tiled=True),
        lax.all_gather(key_rope, "sp", axis=0, tiled=True),
    )
    rows_in = pieces[0].shape[0]
    block = math.gcd(rows_in, 1024)

    def step_block(index, inner):
        first = index * block
        bulk = lax.dynamic_slice_in_dim(pieces[0], first, block, 0)
        rope_rows = lax.dynamic_slice_in_dim(pieces[1], first, block, 0)
        bulk = bulk.reshape(block, heads_here, QUERY_KEY_PLAIN + VALUE_HEAD_SIZE)
        return attend_block(
            inner, bulk[..., :QUERY_KEY_PLAIN], bulk[..., QUERY_KEY_PLAIN:], rope_rows
        )

    final_carry = lax.fori_loop(0, rows_in // block, step_block, start_carry)
    denom = final_carry[1]
    accum = final_carry[2]
    mixed = (
        (accum / jnp.transpose(denom)[:, :, None])
        .astype(jnp.bfloat16)
        .reshape(tokens_here, heads_here * VALUE_HEAD_SIZE)
    )
    up_own = lax.all_to_all(feed_up, "sp", split_axis=1, concat_axis=0, tiled=True)
    down_own = lax.all_to_all(feed_down, "sp", split_axis=0, concat_axis=1, tiled=True)
    share = tokens_here // lax.axis_size("tp")
    lead = lax.axis_index("tp") * share
    branch = lax.psum_scatter(
        jnp.dot(mixed, out_proj, preferred_element_type=jnp.float32).astype(jnp.bfloat16),
        "tp",
        scatter_dimension=0,
        tiled=True,
    ).astype(jnp.float32)
    hidden_own = lax.dynamic_slice_in_dim(hidden_in, lead, share, 0)
    middle_own = (hidden_own.astype(jnp.float32) + branch).astype(jnp.bfloat16)
    normed_own = normalize(middle_own, feed_gain).astype(jnp.bfloat16)
    normed = lax.all_gather(normed_own, ("sp", "tp"), axis=0, tiled=True)
    upward = jnp.dot(normed, up_own, preferred_element_type=jnp.float32)
    activated = jnp.square(jax.nn.relu(upward)).astype(jnp.bfloat16)
    partial_sum = jnp.dot(activated, down_own, preferred_element_type=jnp.float32)
    feed = lax.psum_scatter(
        partial_sum.astype(jnp.bfloat16), ("sp", "tp"), scatter_dimension=0, tiled=True
    ).astype(jnp.float32)
    return (middle_own.astype(jnp.float32) + feed).astype(jnp.bfloat16)


def solution(mesh):
    return jax.shard_map(
        on_device,
        mesh=mesh,
        in_specs=(
            P(("grp", "sp"), None),
            P(("grp", "sp"), None),
            P(("grp", "sp"), None),
            P(("grp", "sp"), None),
            P(),
            P(),
            P(None, "tp"),
            P(None, "tp"),
            P("tp", None),
            P(),
            P("sp", "tp"),
            P("tp", "sp"),
        ),
        out_specs=P(("grp", "sp", "tp"), None),
        check_vma=False,
    )
```

```python
import math

import jax
import jax.numpy as jnp
from jax import lax
from jax.experimental import pallas as pl
from jax.experimental.pallas import tpu as pltpu
from jax.sharding import PartitionSpec as P

QUERY_KEY_PLAIN = 64
QUERY_KEY_ROTARY = 32
VALUE_HEAD_SIZE = 64


def normalize(values, gain):
    floats = values.astype(jnp.float32)
    return floats * lax.rsqrt(jnp.mean(floats * floats, axis=-1, keepdims=True) + 1e-06) * gain


def rotate(values, position):
    half_size = values.shape[-1] // 2
    inverse = 10000.0 ** (-jnp.arange(half_size, dtype=jnp.float32) * 2.0 / values.shape[-1])
    angles = position[:, None] * inverse[None, :]
    cosine = jnp.concatenate([jnp.cos(angles), jnp.cos(angles)], axis=-1)
    sine = jnp.concatenate([jnp.sin(angles), jnp.sin(angles)], axis=-1)
    shape = (values.shape[0],) + (1,) * (values.ndim - 2) + (values.shape[-1],)
    turned = jnp.concatenate([-values[..., half_size:], values[..., :half_size]], axis=-1)
    return values * cosine.reshape(shape) + turned * sine.reshape(shape)


MESH = pl.DeviceIdType.MESH


def layer_kernel(
    n, heads, qp, qr, lat, wkv, hidden, op, gain, up, down, out,
    lat_all, kv_all, op_pad, mixed, up_all, down_all, part_d, recv_d, middle, norm_all, act, part,
    rf1, c2, rf2, c3, rf3, ss, rs, ls,
):
    g, me, t = lax.axis_index("grp"), lax.axis_index("sp"), lax.axis_index("tp")
    c, x = lax.rem(t, 2), t // 2
    share, width = middle.shape
    rows = share * 4
    rank = wkv.shape[0]
    piece_k = up.shape[0]
    hid = down_all.shape[0]
    half_k, half_h = piece_k // 2, hid // 2
    wide = down.shape[1]
    scale_factor = (QUERY_KEY_PLAIN + QUERY_KEY_ROTARY) ** (-0.5)

    def at_z(k):
        return lax.rem(me + k, n)

    def from_z(k):
        return lax.rem(me - k + n, n)

    def at_tp(cc, xx):
        return {"tp": xx * 2 + cc}

    sib, xpeer, ypeer = at_tp(1 - c, x), at_tp(c, 1 - x), {"grp": 1 - g}
    barrier = pltpu.get_barrier_semaphore()
    for k in range(1, n):
        pl.semaphore_signal(barrier, inc=1, device_id={"sp": at_z(k)}, device_id_type=MESH)
    for peer in (sib, xpeer, at_tp(1 - c, 1 - x), ypeer):
        pl.semaphore_signal(barrier, inc=1, device_id=peer, device_id_type=MESH)
    pl.semaphore_wait(barrier, n + 3)

    names = {}
    sent = []

    def slot(name):
        if name not in names:
            names[name] = len(names)
        return names[name]

    def send(name, src, dst, dev):
        i = slot(name)
        copy = pltpu.make_async_remote_copy(
            src_ref=src, dst_ref=dst, send_sem=ss.at[i], recv_sem=rs.at[i],
            device_id=dev, device_id_type=MESH,
        )
        copy.start()
        sent.append(copy)

    def land(name, dst):
        i = slot(name)
        pltpu.make_async_remote_copy(
            src_ref=dst, dst_ref=dst, send_sem=ss.at[i], recv_sem=rs.at[i],
            device_id=sib, device_id_type=MESH,
        ).wait_recv()

    def up_half(owner, hv):
        return up_all.at[pl.ds(pl.multiple_of(owner * piece_k + hv * half_k, half_k), half_k)]

    def down_half(owner, hv):
        return down_all.at[
            pl.ds(pl.multiple_of(hv * half_h, half_h), half_h),
            pl.ds(pl.multiple_of(owner * wide, wide), wide),
        ]

    def begin(tag, buf):
        own = buf.at[me, c, x]
        for k in range(1, n):
            send((tag, "z", k), own, own, {"sp": at_z(k)})
        send((tag, "x", 0), own, own, xpeer)
        send((tag, "s", 0), own, own, sib)

    def finish(tag, buf):
        for k in range(1, n):
            piece = buf.at[from_z(k), c, x]
            land((tag, "z", k), piece)
            send((tag, "x", k), piece, piece, xpeer)
            send((tag, "s", k), piece, piece, sib)
        for k in range(n):
            piece = buf.at[from_z(k), c, 1 - x]
            land((tag, "x", k), piece)
            send((tag, "t", k), piece, piece, sib)
        for k in range(n):
            land((tag, "s", k), buf.at[from_z(k), 1 - c, x])
            land((tag, "t", k), buf.at[from_z(k), 1 - c, 1 - x])

    def send_down(k):
        send(
            ("dn", k),
            down.at[pl.ds(pl.multiple_of(at_z(k) * hid + g * half_h, half_h), half_h)],
            down_half(me, g),
            {"sp": at_z(k)},
        )

    lat_all[me, c, x] = lat[...]
    begin("l", lat_all)
    for k in range(1, n):
        send(
            ("up", k),
            up.at[
                pl.ds(pl.multiple_of(g * half_k, half_k), half_k),
                pl.ds(pl.multiple_of(at_z(k) * hid, hid), hid),
            ],
            up_half(me, g),
            {"sp": at_z(k)},
        )
    for k in range(1, n):
        send_down(k)
    local = [
        pltpu.make_async_copy(
            up.at[:, pl.ds(pl.multiple_of(me * hid, hid), hid)],
            up_all.at[pl.ds(pl.multiple_of(me * piece_k, piece_k), piece_k)],
            ls.at[0],
        ),
        pltpu.make_async_copy(
            down.at[pl.ds(pl.multiple_of(me * hid, hid), hid)],
            down_all.at[:, pl.ds(pl.multiple_of(me * wide, wide), wide)],
            ls.at[1],
        ),
    ]
    for copy in local:
        copy.start()
    vh = VALUE_HEAD_SIZE
    unit = QUERY_KEY_PLAIN + vh
    for h in range(heads):
        op_pad[h * unit : h * unit + QUERY_KEY_PLAIN] = jnp.zeros((QUERY_KEY_PLAIN, width), op.dtype)
        op_pad[h * unit + QUERY_KEY_PLAIN : (h + 1) * unit] = op[h * vh : (h + 1) * vh]
    finish("l", lat_all)
    for j in range(n):
        kv_all[j] = jnp.dot(
            lat_all[j, :, :, :, :rank].reshape(rows, rank),
            wkv[...],
            preferred_element_type=jnp.float32,
        ).astype(jnp.bfloat16)

    contract = (((1,), (1,)), ((), ()))
    rope = lat_all[:, :, :, :, rank:].reshape(n * rows, -1)
    for h in range(heads):
        kv = kv_all[:, :, h * unit : (h + 1) * unit].reshape(n * rows, unit)
        scores = lax.dot_general(qp[h], kv, contract, preferred_element_type=jnp.float32)
        scores += lax.dot_general(qr[h], rope, contract, preferred_element_type=jnp.float32)
        scores = scores * scale_factor
        expo = jnp.exp(scores - jnp.max(scores, axis=-1, keepdims=True))
        total = jnp.sum(expo, axis=-1, keepdims=True)
        mix = jnp.dot(expo.astype(jnp.bfloat16), kv, preferred_element_type=jnp.float32)
        mixed[:, h * unit : (h + 1) * unit] = (mix / total).astype(jnp.bfloat16)

    tile = math.gcd(width, 512)

    @pl.loop(0, width // tile)
    def _(j):
        cols = pl.ds(pl.multiple_of(j * tile, tile), tile)
        part_d[:, cols] = jnp.dot(
            mixed[...], op_pad[:, cols], preferred_element_type=jnp.float32
        ).astype(jnp.bfloat16)

    def own_rows(cc, xx):
        return pl.ds(pl.multiple_of((xx * 2 + cc) * share, share), share)

    others = ((c, 1 - x), (1 - c, 1 - x), (1 - c, x))
    for j, (cc, xx) in enumerate(others):
        send(("d", j), part_d.at[own_rows(cc, xx)], recv_d.at[j], at_tp(cc, xx))
    branch = part_d[own_rows(c, x)].astype(jnp.float32)
    for j in range(3):
        land(("d", j), recv_d.at[j])
        branch += recv_d[j].astype(jnp.float32)
    middle[...] = (hidden[own_rows(c, x)].astype(jnp.float32) + branch).astype(jnp.bfloat16)
    norm_all[me, c, x] = normalize(middle[...], gain[...]).astype(jnp.bfloat16)

    begin("n", norm_all)
    for k in range(1, n):
        piece = up_half(from_z(k), g)
        land(("up", k), piece)
        send(("uy", k), piece, piece, ypeer)
    for k in range(1, n):
        piece = down_half(from_z(k), g)
        land(("dn", k), piece)
        send(("dy", k), piece, piece, ypeer)
    finish("n", norm_all)
    for k in range(1, n):
        land(("uy", k), up_half(from_z(k), 1 - g))
    local[0].wait()
    @pl.loop(0, n)
    def _(j):
        upward = jnp.dot(
            norm_all[j].reshape(rows, width), up_all[...], preferred_element_type=jnp.float32
        )
        act[j] = jnp.square(jnp.maximum(upward, 0.0)).astype(jnp.bfloat16)

    for k in range(1, n):
        land(("dy", k), down_half(from_z(k), 1 - g))
    local[1].wait()

    order = [*range(1, n), 0]
    for k in order:
        dest = at_z(k)

        @pl.loop(0, width // tile)
        def _(j):
            cols = pl.ds(pl.multiple_of(j * tile, tile), tile)
            made = jnp.dot(act[dest], down_all[:, cols], preferred_element_type=jnp.float32)
            part[k, :, :, :, cols] = made.astype(jnp.bfloat16).reshape(2, 2, share, tile)

        send(("f1", k), part.at[k, 1 - c], rf1.at[k], sib)
    for k in order:
        land(("f1", k), rf1.at[k])
        c2[k] = (
            part[k, c, 1 - x].astype(jnp.float32) + rf1[k, 1 - x].astype(jnp.float32)
        ).astype(jnp.bfloat16)
        send(("f2", k), c2.at[k], rf2.at[k], xpeer)
    for k in order:
        land(("f2", k), rf2.at[k])
        c3[k] = (
            part[k, c, x].astype(jnp.float32)
            + rf1[k, x].astype(jnp.float32)
            + rf2[k].astype(jnp.float32)
        ).astype(jnp.bfloat16)
        if k:
            send(("f3", k), c3.at[k], rf3.at[k], {"sp": at_z(k)})
    feed = c3[0].astype(jnp.float32)
    for k in range(1, n):
        land(("f3", k), rf3.at[k])
        feed += rf3[k].astype(jnp.float32)
    out[...] = (middle[...].astype(jnp.float32) + feed).astype(jnp.bfloat16)
    for copy in sent:
        copy.wait_send()


def run_layer(
    queries, latent, key_rope, key_value_up_weight, hidden_in, out_proj, feed_gain, feed_up, feed_down
):
    n = lax.axis_size("sp")
    rows, heads, size = queries.shape
    width = hidden_in.shape[1]
    share = rows // lax.axis_size("tp")
    hid = feed_up.shape[1] // n
    turned = jnp.transpose(queries, (1, 0, 2))
    unit = QUERY_KEY_PLAIN + VALUE_HEAD_SIZE
    plain = jnp.pad(turned[..., :QUERY_KEY_PLAIN], ((0, 0), (0, 0), (0, VALUE_HEAD_SIZE)))
    rotary = jnp.pad(turned[..., QUERY_KEY_PLAIN:], ((0, 0), (0, 0), (0, unit - QUERY_KEY_ROTARY)))
    lat = jnp.concatenate(
        [latent, jnp.pad(key_rope, ((0, 0), (0, unit - QUERY_KEY_ROTARY)))], axis=1
    )
    lat = lax.dynamic_slice_in_dim(lat, lax.axis_index("tp") * share, share, 0)
    bf = jnp.bfloat16
    vmem = pl.BlockSpec(memory_space=pltpu.VMEM)
    anywhere = pl.BlockSpec(memory_space=pl.ANY)
    copies = 16 * n
    block = (share, width)
    return pl.pallas_call(
        lambda *refs: layer_kernel(n, heads, *refs),
        out_shape=jax.ShapeDtypeStruct(block, bf),
        in_specs=[vmem] * 7 + [anywhere] * 2,
        out_specs=vmem,
        scratch_shapes=[
            pltpu.VMEM((n, 2, 2, *lat.shape), bf),
            pltpu.VMEM((n, rows, heads * unit), bf),
            pltpu.VMEM((heads * unit, width), bf),
            pltpu.VMEM((rows, heads * unit), bf),
            pltpu.VMEM((feed_up.shape[0] * n, hid), bf),
            pltpu.VMEM((hid, feed_down.shape[1] * n), bf),
            pltpu.VMEM((rows, width), bf),
            pltpu.VMEM((3, *block), bf),
            pltpu.VMEM(block, bf),
            pltpu.VMEM((n, 2, 2, *block), bf),
            pltpu.VMEM((n, rows, hid), bf),
            pltpu.VMEM((n, 2, 2, *block), bf),
            pltpu.VMEM((n, 2, *block), bf),
            pltpu.VMEM((n, *block), bf),
            pltpu.VMEM((n, *block), bf),
            pltpu.VMEM((n, *block), bf),
            pltpu.VMEM((n, *block), bf),
            pltpu.SemaphoreType.DMA((copies,)),
            pltpu.SemaphoreType.DMA((copies,)),
            pltpu.SemaphoreType.DMA((2,)),
        ],
        compiler_params=pltpu.CompilerParams(
            collective_id=0, has_side_effects=True, vmem_limit_bytes=60 * 1024 * 1024
        ),
    )(
        plain, rotary, lat, key_value_up_weight, hidden_in, out_proj,
        feed_gain.reshape(1, -1), feed_up, feed_down,
    )


def fits_kernel(tokens, feed_up):
    n = lax.axis_size("sp")
    hid = feed_up.shape[1] // n
    return (
        lax.axis_size("grp") == 2
        and lax.axis_size("tp") == 4
        and 1 < n
        and tokens * n <= 1024
        and tokens % 64 == 0
        and hid % 128 == 0
        and hid <= 512
    )


def on_device(
    hidden_in,
    query_latent_rows,
    key_value_latent,
    rotary_key,
    query_norm_gain,
    key_value_gain,
    query_up_weight,
    key_value_up_weight,
    out_proj,
    feed_gain,
    feed_up,
    feed_down,
):
    tokens_here = hidden_in.shape[0]
    heads_here = query_up_weight.shape[1] // (QUERY_KEY_PLAIN + QUERY_KEY_ROTARY)
    position = (lax.axis_index("sp") * tokens_here + jnp.arange(tokens_here)).astype(jnp.float32)
    scale_factor = (QUERY_KEY_PLAIN + QUERY_KEY_ROTARY) ** (-0.5)
    query_norm = normalize(query_latent_rows, query_norm_gain).astype(jnp.bfloat16)
    queries = jnp.dot(query_norm, query_up_weight, preferred_element_type=jnp.float32).reshape(
        tokens_here, heads_here, QUERY_KEY_PLAIN + QUERY_KEY_ROTARY
    )
    queries = jnp.concatenate(
        [queries[..., :QUERY_KEY_PLAIN], rotate(queries[..., QUERY_KEY_PLAIN:], position)], axis=-1
    ).astype(jnp.bfloat16)
    query_plain = queries[..., :QUERY_KEY_PLAIN]
    query_turned = queries[..., QUERY_KEY_PLAIN:]
    latent = normalize(key_value_latent, key_value_gain).astype(jnp.bfloat16)
    key_rope = rotate(rotary_key.astype(jnp.float32), position).astype(jnp.bfloat16)

    def attend_block(carry, key_plain, value_rows, rope_rows):
        row_max, denom, accum = carry
        scores = jnp.einsum(
            "qhd,khd->hqk", query_plain, key_plain, preferred_element_type=jnp.float32
        )
        scores = scores + jnp.einsum(
            "qhd,kd->hqk", query_turned, rope_rows, preferred_element_type=jnp.float32
        )
        scores = scores * scale_factor
        new_max = jnp.maximum(row_max, jnp.max(scores, axis=-1))
        expo = jnp.exp(scores - new_max[:, :, None])
        factor = jnp.exp(row_max - new_max)
        denom = denom * factor + jnp.sum(expo, axis=-1)
        update = jnp.einsum(
            "hqk,khd->qhd",
            expo.astype(jnp.bfloat16),
            value_rows,
            preferred_element_type=jnp.float32,
        )
        accum = accum * jnp.transpose(factor)[:, :, None] + update
        return (new_max, denom, accum)

    start_carry = (
        jnp.full((heads_here, tokens_here), -1e30, jnp.float32),
        jnp.zeros((heads_here, tokens_here), jnp.float32),
        jnp.zeros((tokens_here, heads_here, VALUE_HEAD_SIZE), jnp.float32),
    )
    own_keys = jnp.dot(latent, key_value_up_weight, preferred_element_type=jnp.float32).astype(
        jnp.bfloat16
    )
    if fits_kernel(tokens_here, feed_up):
        return run_layer(
            queries, latent, key_rope, key_value_up_weight, hidden_in, out_proj,
            feed_gain, feed_up, feed_down,
        )
    pieces = (
        lax.all_gather(own_keys, "sp", axis=0, tiled=True),
        lax.all_gather(key_rope, "sp", axis=0, tiled=True),
    )
    rows_in = pieces[0].shape[0]
    block = math.gcd(rows_in, 1024)

    def step_block(index, inner):
        first = index * block
        bulk = lax.dynamic_slice_in_dim(pieces[0], first, block, 0)
        rope_rows = lax.dynamic_slice_in_dim(pieces[1], first, block, 0)
        bulk = bulk.reshape(block, heads_here, QUERY_KEY_PLAIN + VALUE_HEAD_SIZE)
        return attend_block(
            inner, bulk[..., :QUERY_KEY_PLAIN], bulk[..., QUERY_KEY_PLAIN:], rope_rows
        )

    final_carry = lax.fori_loop(0, rows_in // block, step_block, start_carry)
    denom = final_carry[1]
    accum = final_carry[2]
    mixed = (
        (accum / jnp.transpose(denom)[:, :, None])
        .astype(jnp.bfloat16)
        .reshape(tokens_here, heads_here * VALUE_HEAD_SIZE)
    )
    up_own = lax.all_to_all(feed_up, "sp", split_axis=1, concat_axis=0, tiled=True)
    down_own = lax.all_to_all(feed_down, "sp", split_axis=0, concat_axis=1, tiled=True)
    share = tokens_here // lax.axis_size("tp")
    lead = lax.axis_index("tp") * share
    branch = lax.psum_scatter(
        jnp.dot(mixed, out_proj, preferred_element_type=jnp.float32).astype(jnp.bfloat16),
        "tp",
        scatter_dimension=0,
        tiled=True,
    ).astype(jnp.float32)
    hidden_own = lax.dynamic_slice_in_dim(hidden_in, lead, share, 0)
    middle_own = (hidden_own.astype(jnp.float32) + branch).astype(jnp.bfloat16)
    normed_own = normalize(middle_own, feed_gain).astype(jnp.bfloat16)
    normed = lax.all_gather(normed_own, ("sp", "tp"), axis=0, tiled=True)
    upward = jnp.dot(normed, up_own, preferred_element_type=jnp.float32)
    activated = jnp.square(jax.nn.relu(upward)).astype(jnp.bfloat16)
    partial_sum = jnp.dot(activated, down_own, preferred_element_type=jnp.float32)
    feed = lax.psum_scatter(
        partial_sum.astype(jnp.bfloat16), ("sp", "tp"), scatter_dimension=0, tiled=True
    ).astype(jnp.float32)
    return (middle_own.astype(jnp.float32) + feed).astype(jnp.bfloat16)


def solution(mesh):
    return jax.shard_map(
        on_device,
        mesh=mesh,
        in_specs=(
            P(("grp", "sp"), None),
            P(("grp", "sp"), None),
            P(("grp", "sp"), None),
            P(("grp", "sp"), None),
            P(),
            P(),
            P(None, "tp"),
            P(None, "tp"),
            P("tp", None),
            P(),
            P("sp", "tp"),
            P("tp", "sp"),
        ),
        out_specs=P(("grp", "sp", "tp"), None),
        check_vma=False,
    )
```
